512 devices in a mesh: fs: 16 (over y, x), tp: 32 (over z, core).
Axes of the slice: x: 4, y: 4, z: 16, core: 2. Of those that a mesh axis runs over, the one named last changes fastest.
Arguments:
- value_input: bfloat16 [32768, 2048], P('fs', 'tp'), may hold values from -50 to 50
- value_cotangent: bfloat16 [32768, 512], P('fs'), may hold values from -6 to 6
- value_factor: bfloat16 [512, 128], replicated, may hold values from -10 to 10
- value_master: float32 [512, 2048], P('fs', 'tp'), may hold values from -0.125 to 0.125
- value_first: float32 [128, 2048], P('fs', 'tp'), may hold values from -4 to 4
- value_second: float32 [128, 2048], P('fs', 'tp'), may hold values from 0.01 to 0.2
- mixed_heads: bfloat16 [32768, 1024], P('fs', 'tp'), may hold values from -6 to 6
- output_cotangent: bfloat16 [32768, 2048], P('fs', 'tp'), may hold values from -50 to 50
- output_factor: bfloat16 [1024, 128], replicated, may hold values from -10 to 10
- output_master: float32 [1024, 2048], P('fs', 'tp'), may hold values from -0.1875 to 0.1875
- output_first: float32 [128, 2048], P('fs', 'tp'), may hold values from -4 to 4
- output_second: float32 [128, 2048], P('fs', 'tp'), may hold values from 0.01 to 0.2
Outputs:
- value_step: float32 [512, 2048], P('fs', 'tp')
- value_new_master: float32 [512, 2048], P('fs', 'tp')
- value_copy: bfloat16 [512, 2048], P(None, 'tp')
- value_first_new: float32 [128, 2048], P('fs', 'tp')
- value_second_new: float32 [128, 2048], P('fs', 'tp')
- output_step: float32 [1024, 2048], P('fs', 'tp')
- output_new_master: float32 [1024, 2048], P('fs', 'tp')
- output_copy: bfloat16 [1024, 2048], P(None, 'tp')
- output_first_new: float32 [128, 2048], P('fs', 'tp')
- output_second_new: float32 [128, 2048], P('fs', 'tp')
The draws below stay inside these ranges and needn't reach their ends.
All inputs are finite; a program needn't handle non-finite values.
Results may differ from the reference program's by a relative error of at most 0.001.
Values may be sent and summed in bfloat16 or wider, within the bound.
A program may use at most 64 MiB of HBM per device.

```python
import math
import jax
import jax.numpy as jnp
from jax import lax

D = 2048
RANK = 128
HW = 1024
VW = 512
TOKENS = 32768


def column_scaled(key, rows, cols):
    key_rough, key_own = jax.random.split(key, 2)
    ramp = 10.0 ** (jnp.arange(cols, dtype=jnp.float32) / (cols - 1))
    rough = jnp.exp(jax.random.uniform(key_rough, (cols,), jnp.float32, -0.35, 0.35))
    base = jnp.clip(jax.random.normal(key_own, (rows, cols), jnp.float32), -3.5, 3.5)
    return base * ramp[None, :] * rough[None, :]


def draw_value_input(key, part):
    return column_scaled(jax.random.fold_in(key, 11), TOKENS, D).astype(jnp.bfloat16)


def draw_output_cotangent(key, part):
    return column_scaled(jax.random.fold_in(key, 12), TOKENS, D).astype(jnp.bfloat16)


def draw_value_factor(key, part):
    return (column_scaled(jax.random.fold_in(key, 13), VW, RANK) * VW ** (-0.5)).astype(jnp.bfloat16)


def draw_output_factor(key, part):
    return (column_scaled(jax.random.fold_in(key, 14), HW, RANK) * HW ** (-0.5)).astype(jnp.bfloat16)


def level_of(rng, dims, shards, least, largest):
    gain = 1.0
    for position, parts in shards:
        draws = jax.random.uniform(jax.random.fold_in(jax.random.fold_in(rng, 6), position), (parts,), jnp.float32, least / len(shards), largest / len(shards))
        gain = gain * jnp.repeat(jnp.exp(draws), dims[position] // parts).reshape((-1,) + (1,) * (len(dims) - 1 - position))
    return gain


def scatter_about(own_key, dims, scale, bound, cuts=(), kind=jnp.bfloat16):
    result = jax.random.normal(own_key, dims, jnp.float32) * scale
    if len(cuts) > 0:
        result = level_of(own_key, dims, cuts, -0.22, 0.18) * result
    return jnp.clip(result, min=-bound, max=bound).astype(kind)


def setup_inputs(seed: int = 0) -> dict:
    splits = jax.random.split(jax.random.key(seed), 13)
    value_input = draw_value_input(jax.random.fold_in(splits[12], 71), 0)
    value_cotangent = scatter_about(splits[1], (TOKENS, VW), 1.0, 6.0, ((0, 16),))
    value_factor = draw_value_factor(jax.random.fold_in(splits[12], 71), 0)
    value_master = scatter_about(splits[3], (VW, D), D ** -0.5, 0.125, ((0, 16), (1, 32)), jnp.float32)
    value_first = scatter_about(splits[4], (RANK, D), 0.3, 4.0, ((0, 16), (1, 32)), jnp.float32)
    value_second = jnp.clip(jnp.exp(math.log(0.2) - 2.9957323 * jax.random.uniform(splits[5], (RANK, D), jnp.float32) ** level_of(splits[5], (RANK, D), ((0, 16), (1, 32)), -0.2, 0.2)), 0.01, 0.2)
    mixed_heads = scatter_about(splits[6], (TOKENS, HW), 1.0, 6.0, ((0, 16), (1, 32)))
    output_cotangent = draw_output_cotangent(jax.random.fold_in(splits[12], 71), 0)
    output_factor = draw_output_factor(jax.random.fold_in(splits[12], 71), 0)
    output_master = scatter_about(splits[9], (HW, D), HW ** -0.5, 0.1875, ((0, 16), (1, 32)), jnp.float32)
    output_first = scatter_about(splits[10], (RANK, D), 0.3, 4.0, ((0, 16), (1, 32)), jnp.float32)
    output_second = jnp.clip(jnp.exp(math.log(0.2) - 2.9957323 * jax.random.uniform(splits[11], (RANK, D), jnp.float32) ** level_of(splits[11], (RANK, D), ((0, 16), (1, 32)), -0.2, 0.2)), 0.01, 0.2)
    return {"value_input": value_input, "value_cotangent": value_cotangent, "value_factor": value_factor, "value_master": value_master, "value_first": value_first, "value_second": value_second, "mixed_heads": mixed_heads, "output_cotangent": output_cotangent, "output_factor": output_factor, "output_master": output_master, "output_first": output_first, "output_second": output_second}


highest = lax.Precision.HIGHEST

def adam_part(projected, first, second, factor, master):
    scale = lax.rsqrt(jnp.mean(projected * projected) + 1e-06)
    scaled = scale * projected
    first_new = 0.9 * first + 0.1 * scaled
    second_new = 0.95 * second + 0.05 * scaled * scaled
    direction = first_new / (jnp.sqrt(second_new) + 1e-08)
    step = jnp.dot(factor.astype(jnp.float32), direction, precision=highest, preferred_element_type=jnp.float32)
    new_master = master - 0.002 * step
    return (step, new_master, new_master.astype(jnp.bfloat16), first_new, second_new)

def reference(value_input, value_cotangent, value_factor, value_master, value_first, value_second, mixed_heads, output_cotangent, output_factor, output_master, output_first, output_second):
    value_image = jnp.dot(value_cotangent.astype(jnp.float32), value_factor.astype(jnp.float32), precision=highest, preferred_element_type=jnp.float32)
    value_projected = jnp.dot(value_image.T, value_input.astype(jnp.float32), precision=highest, preferred_element_type=jnp.float32)
    output_image = jnp.dot(mixed_heads.astype(jnp.float32), output_factor.astype(jnp.float32), precision=highest, preferred_element_type=jnp.float32)
    output_projected = jnp.dot(output_image.T, output_cotangent.astype(jnp.float32), precision=highest, preferred_element_type=jnp.float32)
    value_out = adam_part(value_projected, value_first, value_second, value_factor, value_master)
    output_out = adam_part(output_projected, output_first, output_second, output_factor, output_master)
    return (value_out[0], value_out[1], value_out[2], value_out[3], value_out[4], output_out[0], output_out[1], output_out[2], output_out[3], output_out[4])
```

```python
import functools

import jax
import jax.numpy as jnp
from jax import lax
from jax.experimental import pallas as pl
from jax.experimental.pallas import tpu as pltpu
from jax.sharding import PartitionSpec as P

MESH = pl.DeviceIdType.MESH
f32 = jnp.float32
bf16 = jnp.bfloat16
NT = (((1,), (1,)), ((), ()))


def two_parts(x):
    hi = x.astype(bf16)
    return hi, (x - hi.astype(f32)).astype(bf16)


def dot(a, b):
    return jnp.dot(a, b, preferred_element_type=f32)


def dot_nt(a, b):
    return lax.dot_general(a, b, NT, preferred_element_type=f32)


def exact_dot(x, w):
    hi, lo = two_parts(x)
    return dot(hi, w) + dot(lo, w)


def rcopy(src, dst, send, recv, device):
    return pltpu.make_async_remote_copy(
        src_ref=src,
        dst_ref=dst,
        send_sem=send,
        recv_sem=recv,
        device_id=device,
        device_id_type=MESH,
    )


def main_kernel(
    nf,
    nz,
    total_count,
    vi_h,
    vc_h,
    fv_h,
    vm_h,
    vf_h,
    vs_h,
    mh_h,
    oc_h,
    fo_h,
    om_h,
    of_h,
    os_h,
    vstep_o,
    vnew_o,
    vcopy_o,
    vfirst_o,
    vsecond_o,
    ostep_o,
    onew_o,
    ocopy_o,
    ofirst_o,
    osecond_o,
    heads,
    vi,
    vc,
    fv,
    vm,
    vf,
    vs,
    oc,
    fo,
    om,
    of,
    os_,
    packs,
    acc,
    part_v,
    part_o,
    rs_v,
    rs_o,
    ag_v,
    ag_o,
    zrow,
    mt_v,
    mt_o,
    mom,
    pt_full,
    load_sem,
    ring_send,
    ring_recv,
    pn_send,
    pn_recv,
    fs_send,
    fs_recv,
    z_send,
    z_recv,
):
    me_f = lax.axis_index("fs")
    me_t = lax.axis_index("tp")
    z = me_t // 2
    core = lax.rem(me_t, 2)
    other = 1 - core
    half = nz // 2
    right = (me_f, lax.rem(z + 1, nz) * 2 + core)
    left = (me_f, lax.rem(z + nz - 1, nz) * 2 + core)
    partner = (me_f, z * 2 + other)

    def fs_dev(k):
        return lax.rem(me_f + k, nf)

    pairs = [
        (mh_h.at[0], heads.at[z, core, 0]),
        (mh_h.at[1], heads.at[z, core, 1]),
        (vf_h, vf),
        (vs_h, vs),
        (of_h, of),
        (os_h, os_),
        (vm_h, vm),
        (om_h, om),
        (vi_h, vi),
        (vc_h, vc),
        (fv_h, fv),
        (oc_h, oc),
        (fo_h, fo),
    ]
    loads = [pltpu.make_async_copy(s, d, load_sem.at[n]) for n, (s, d) in enumerate(pairs)]
    for cp in loads:
        cp.start()

    barrier = pltpu.get_barrier_semaphore()
    for dev in (left, right, partner):
        pl.semaphore_signal(barrier, inc=1, device_id=dev, device_id_type=MESH)
    for k in range(1, nf):
        pl.semaphore_signal(barrier, inc=1, device_id=(fs_dev(k), me_t), device_id_type=MESH)
    pl.semaphore_wait(barrier, 3 + nf - 1)

    def chip_at(d, s):
        return lax.rem(z + (nz - s if d == 0 else s), nz)

    def has(s, c, d):
        return s < half or c == d

    def ring_out(d, s, c):
        ref = heads.at[chip_at(d, s - 1), core, c]
        dev = right if d == 0 else left
        return rcopy(ref, ref, ring_send.at[d, s - 1, c], ring_recv.at[d, s - 1, c], dev)

    def ring_in(d, s, c):
        ref = heads.at[chip_at(d, s), core, c]
        dev = right if d == 0 else left
        return rcopy(ref, ref, ring_send.at[d, s - 1, c], ring_recv.at[d, s - 1, c], dev)

    def pn_out(d, s, c):
        ref = heads.at[chip_at(d, s), core, c]
        return rcopy(ref, ref, pn_send.at[d, s, c], pn_recv.at[d, s, c], partner)

    def pn_in(d, s, c):
        ref = heads.at[chip_at(d, s), other, c]
        return rcopy(ref, ref, pn_send.at[d, s, c], pn_recv.at[d, s, c], partner)

    sent = []

    def send(cp):
        cp.start()
        sent.append(cp)

    for c in range(2):
        loads[c].wait()
        for d in range(2):
            send(ring_out(d, 1, c))
    for c in range(2):
        send(pn_out(0, 0, c))

    for n in range(2, 8):
        loads[n].wait()
    own_v = jnp.concatenate([vf[...], vs[...], of[...], os_[...], vm[...]], axis=0)
    packs[me_f] = jnp.concatenate([own_v, om[...]], axis=1)

    def exchange(n, src, dst):
        for k in range(1, nf):
            send(rcopy(src(k), dst.at[me_f], fs_send.at[n, k], fs_recv.at[n, k], (fs_dev(k), me_t)))

    def arrive(n, dst):
        for k in range(1, nf):
            ref = dst.at[lax.rem(me_f + nf - k, nf)]
            rcopy(ref, ref, fs_send.at[n, k], fs_recv.at[n, k], (fs_dev(k), me_t)).wait_recv()

    exchange(0, lambda k: packs.at[me_f], packs)

    def scatter(n, part, rs, value):
        for i in range(nf):
            part[i] = value[4 * i : 4 * i + 4]
        rs[me_f] = part[me_f]
        exchange(n, lambda k: part.at[fs_dev(k)], rs)

    def gather(n, rs, ag):
        band = rs[0]
        for i in range(1, nf):
            band = band + rs[i]
        ag[me_f] = band
        exchange(n, lambda k: ag.at[me_f], ag)

    for n in range(8, 11):
        loads[n].wait()
    gv = dot(vi[...], vc[...])
    scatter(1, part_v, rs_v, exact_dot(gv, fv[...]))
    for n in range(11, 13):
        loads[n].wait()
    acc[...] = jnp.zeros_like(acc)

    def contribute(d, s):
        chip = chip_at(d, s)
        block = heads[chip].reshape(64, heads.shape[-1])
        g = dot_nt(oc[...], block)
        acc[...] += exact_dot(g, fo[pl.ds(pl.multiple_of(chip * 64, 64), 64), :])

    def partner_arrived(s):
        for c in range(2):
            for d in range(2):
                if (s > 0 or d == 0) and has(s, c, d):
                    pn_in(d, s, c).wait_recv()

    for s in range(1, half + 1):
        for c in range(2):
            for d in range(2):
                if has(s, c, d):
                    ring_in(d, s, c).wait_recv()
                    if s < half and has(s + 1, c, d):
                        send(ring_out(d, s + 1, c))
                    send(pn_out(d, s, c))
        partner_arrived(s - 1)
        contribute(0, s - 1)
        if s > 1:
            contribute(1, s - 1)
        if s == 2:
            arrive(1, rs_v)
            gather(2, rs_v, ag_v)
        if s == 3:
            arrive(0, packs)
            mt_v[...] = packs[:, 32:64, 0:64].reshape(nf * 32, 64).T
        if s == 4:
            mt_o[...] = packs[:, :, 64:128].reshape(nf * 64, 64).T
        if s == 5:
            for n in range(4):
                mom[n] = packs[:, 8 * n : 8 * n + 8, 0:64].reshape(nf * 8, 64).T
        if s == 6:
            arrive(2, ag_v)
    partner_arrived(half)
    contribute(0, half)

    scatter(3, part_o, rs_o, acc[...])
    arrive(3, rs_o)
    gather(4, rs_o, ag_o)
    arrive(4, ag_o)

    def whole(ag):
        return jnp.concatenate([ag[i] for i in range(nf)], axis=0)

    pv = whole(ag_v)
    po = whole(ag_o)

    def folded(p):
        row = jnp.sum(p * p, axis=0, keepdims=True)
        return row[:, :64] + row[:, 64:]

    zrow[me_t] = jnp.concatenate([folded(pv), folded(po)], axis=1)
    order = sorted(range(1, 2 * nz), key=lambda k: -min(k, 2 * nz - k))
    for k in order:
        dev = (me_f, lax.rem(me_t + k, 2 * nz))
        send(rcopy(zrow.at[me_t], zrow.at[me_t], z_send.at[k], z_recv.at[k], dev))
    pt_full[0] = pv.T
    pt_full[1] = po.T
    at8 = pl.ds(pl.multiple_of(me_f * 8, 8), 8)
    band_v = pt_full[0, at8, :]
    band_o = pt_full[1, at8, :]
    for k in order:
        ref = zrow.at[lax.rem(me_t + 2 * nz - k, 2 * nz)]
        dev = (me_f, lax.rem(me_t + k, 2 * nz))
        rcopy(ref, ref, z_send.at[k], z_recv.at[k], dev).wait_recv()
    rows = zrow[0]
    for j in range(1, 2 * nz):
        rows = rows + zrow[j]
    scale_v = lax.rsqrt(jnp.sum(rows[:, :64], axis=1, keepdims=True) / total_count + 1e-06)
    scale_o = lax.rsqrt(jnp.sum(rows[:, 64:], axis=1, keepdims=True) / total_count + 1e-06)

    def update(projected, scale, first, second):
        scaled = scale * projected
        first_new = 0.9 * first + 0.1 * scaled
        second_new = 0.95 * second + 0.05 * scaled * scaled
        return first_new, second_new

    def finish(p, band, scale, n, first, second, factor, mt, master, step_o, new_o, copy_o, first_o, second_o):
        first_new, second_new = update(p, scale, mom[n], mom[n + 1])
        direction = first_new / (jnp.sqrt(second_new) + 1e-08)
        hi, lo = two_parts(direction)
        w = factor[...]
        step_t = dot_nt(hi, w) + dot_nt(lo, w)
        copy_o[...] = (mt[...] - 0.002 * step_t).astype(bf16)
        count = master.shape[0]
        block = factor[pl.ds(pl.multiple_of(me_f * count, count), count), :]
        step = dot_nt(block, hi) + dot_nt(block, lo)
        step_o[...] = step
        new_o[...] = master[...] - 0.002 * step
        first_o[...], second_o[...] = update(band, scale, first[...], second[...])

    finish(pv, band_v, scale_v, 0, vf, vs, fv, mt_v, vm, vstep_o, vnew_o, vcopy_o, vfirst_o, vsecond_o)
    finish(po, band_o, scale_o, 2, of, os_, fo, mt_o, om, ostep_o, onew_o, ocopy_o, ofirst_o, osecond_o)

    for cp in sent:
        cp.wait_send()


def export_kernel(*refs):
    count = (len(refs) - 1) // 2
    ins, outs, sem = refs[:count], refs[count : 2 * count], refs[-1]
    copies = [pltpu.make_async_copy(a, b, sem.at[n]) for n, (a, b) in enumerate(zip(ins, outs))]
    for cp in copies:
        cp.start()
    for cp in copies:
        cp.wait()


def on_device(nf, nz, vi, vc, fv, vm, vf, vs, mh, oc, fo, om, of, os_):
    tokens, columns = vi.shape
    rank = fv.shape[1]
    total_count = rank * columns * nz * 2
    f_rows, o_rows = fv.shape[0], fo.shape[0]

    def out(shape, dtype):
        return jax.ShapeDtypeStruct(shape, dtype)

    outs = (
        out(vm.shape, f32),
        out(vm.shape, f32),
        out((columns, f_rows), bf16),
        out(vf.shape, f32),
        out(vf.shape, f32),
        out(om.shape, f32),
        out(om.shape, f32),
        out((columns, o_rows), bf16),
        out(of.shape, f32),
        out(of.shape, f32),
    )
    V = pltpu.VMEM
    D = pltpu.SemaphoreType.DMA
    half = nz // 2
    scratch = [
        V((nz, 2, 2, 16, tokens), bf16),
        V((columns, tokens), bf16),
        V(vc.shape, bf16),
        V(fv.shape, bf16),
        V(vm.shape, f32),
        V(vf.shape, f32),
        V(vs.shape, f32),
        V((columns, tokens), bf16),
        V(fo.shape, bf16),
        V(om.shape, f32),
        V(of.shape, f32),
        V(os_.shape, f32),
        V((nf, 64, 128), f32),
        V((columns, rank), f32),
        V((nf, 4, 128), f32),
        V((nf, 4, 128), f32),
        V((nf, 4, 128), f32),
        V((nf, 4, 128), f32),
        V((nf, 4, 128), f32),
        V((nf, 4, 128), f32),
        V((2 * nz, 1, 128), f32),
        V((columns, f_rows), f32),
        V((columns, o_rows), f32),
        V((4, columns, rank), f32),
        V((2, rank, columns), f32),
        D((13,)),
        D((2, half, 2)),
        D((2, half, 2)),
        D((2, half + 1, 2)),
        D((2, half + 1, 2)),
        D((5, nf)),
        D((5, nf)),
        D((2 * nz,)),
        D((2 * nz,)),
    ]
    hbm = pl.BlockSpec(memory_space=pltpu.MemorySpace.HBM)
    vmem = pl.BlockSpec(memory_space=pltpu.VMEM)
    results = pl.pallas_call(
        functools.partial(main_kernel, nf, nz, total_count),
        out_shape=outs,
        in_specs=[hbm] * 12,
        out_specs=(vmem,) * 10,
        scratch_shapes=scratch,
        compiler_params=pltpu.CompilerParams(
            collective_id=0, has_side_effects=True, vmem_limit_bytes=32 * 1024 * 1024
        ),
        name="main",
    )(vi.T, vc, fv, vm, vf, vs, mh.T.reshape(2, 16, tokens), oc.T, fo, om, of, os_)
    results = pl.pallas_call(
        export_kernel,
        out_shape=outs,
        in_specs=[vmem] * 10,
        out_specs=(hbm,) * 10,
        scratch_shapes=[D((10,))],
        compiler_params=pltpu.CompilerParams(vmem_limit_bytes=16 * 1024 * 1024),
        name="export",
    )(*results)
    results = list(results)
    results[2] = results[2].T
    results[7] = results[7].T
    return tuple(results)


def solution(mesh):
    both = P("fs", "tp")
    cols = P(None, "tp")
    return jax.shard_map(
        functools.partial(on_device, mesh.shape["fs"], mesh.shape["tp"] // 2),
        mesh=mesh,
        in_specs=(both, P("fs", None), P(), both, both, both, both, both, P(), both, both, both),
        out_specs=(both, both, cols, both, both, both, both, cols, both, both),
        check_vma=False,
    )
```
